32 devices in a mesh: sp: 16 (over z, y, x), dp: 2 (over core).
Axes of the slice: x: 2, y: 2, z: 4, core: 2. Of those that a mesh axis runs over, the one named last changes fastest.
Arguments:
- tokens: bfloat16 [2, 2048, 2048], P('dp', 'sp'), may hold values from -6 to 6
- w_value: bfloat16 [2048, 1024], P('dp', 'sp'), may hold values from -0.125 to 0.125
- w_gate: bfloat16 [2048, 1024], P('dp', 'sp'), may hold values from -0.125 to 0.125
- w_out: bfloat16 [1024, 2048], P('dp', 'sp'), may hold values from -0.1875 to 0.1875
- conv_taps: bfloat16 [1024, 31], replicated, may hold values from -1 to 1
- norm_gain: float32 [1024], replicated, may hold values from 0.1 to 1.9
- norm_bias: float32 [1024], replicated, may hold values from -3 to 3
Outputs:
- mixed: bfloat16 [2, 2048, 2048], P('dp', 'sp')
The draws below stay inside these ranges and needn't reach their ends.
All inputs are finite; a program needn't handle non-finite values.
Results may differ from the reference program's by a relative error of at most 0.0064.
Values may be sent and summed in bfloat16 or wider, within the bound.
A program may use at most 64 MiB of HBM per device.

```python
import jax
import jax.numpy as jnp
from jax import lax

D = 2048
CH = 1024
KW = 31
SEQ = 2048
SEQS = 2


def levels(stream_key, shape, shards, smallest, largest):
    gain = 1.0
    for position, blocks in shards:
        heights = jax.random.uniform(jax.random.fold_in(jax.random.fold_in(stream_key, 6), position), (blocks,), jnp.float32, smallest / len(shards), largest / len(shards))
        gain = gain * jnp.repeat(jnp.exp(heights), shape[position] // blocks).reshape((-1,) + (1,) * (len(shape) - 1 - position))
    return gain


def scatter_about(stream_key, dims, deviation, limit, split=(), held_as=jnp.bfloat16):
    entries = deviation * jax.random.normal(stream_key, dims, jnp.float32)
    if split:
        entries = entries * levels(stream_key, dims, split, -0.22, 0.18)
    return jnp.clip(entries, -limit, limit).astype(held_as)


def setup_inputs(seed: int = 0) -> dict:
    key_list = jax.random.split(jax.random.key(seed), 8)
    tokens = scatter_about(key_list[0], (SEQS, SEQ, D), 1.0, 6.0, ((0, 2), (1, 16)))
    w_value = scatter_about(key_list[1], (D, CH), D ** -0.5, 0.125, ((0, 2), (1, 16)))
    w_gate = scatter_about(key_list[2], (D, CH), D ** -0.5, 0.125, ((0, 2), (1, 16)))
    w_out = scatter_about(key_list[3], (CH, D), CH ** -0.5, 0.1875, ((0, 2), (1, 16)))
    conv_taps = scatter_about(key_list[4], (CH, KW), KW ** -0.5, 1.0)
    norm_gain = jnp.clip(1.0 + 0.18 * jax.random.normal(key_list[5], (CH,), jnp.float32), 0.1, 1.9)
    norm_bias = scatter_about(key_list[6], (CH,), 0.5, 3.0, (), jnp.float32)
    return {"tokens": tokens, "w_value": w_value, "w_gate": w_gate, "w_out": w_out, "conv_taps": conv_taps, "norm_gain": norm_gain, "norm_bias": norm_bias}


def reference(tokens, w_value, w_gate, w_out, conv_taps, norm_gain, norm_bias):
    margin = KW // 2
    taps = conv_taps.astype(jnp.float32).T

    def one_sequence(seq_rows):
        value = jnp.dot(seq_rows, w_value, preferred_element_type=jnp.float32)
        gate = jnp.dot(seq_rows, w_gate, preferred_element_type=jnp.float32)
        gated = lax.optimization_barrier((value * jax.nn.sigmoid(gate)).astype(jnp.bfloat16))
        padded = jnp.pad(gated, ((margin, margin), (0, 0))).astype(jnp.float32)
        total = jnp.zeros((SEQ, CH), jnp.float32)
        for offset in range(KW):
            total = total + padded[offset:offset + SEQ] * taps[offset][None, :]
        conv = lax.optimization_barrier(total.astype(jnp.bfloat16)).astype(jnp.float32)
        mean = lax.optimization_barrier(jnp.mean(conv, axis=-1, keepdims=True))
        centred = conv - mean
        variance = lax.optimization_barrier(jnp.mean(centred * centred, axis=-1, keepdims=True))
        normed = centred * lax.rsqrt(variance + 1e-05) * norm_gain[None, :] + norm_bias[None, :]
        act = (normed * jax.nn.sigmoid(normed)).astype(jnp.bfloat16)
        return jnp.dot(act, w_out, preferred_element_type=jnp.float32).astype(jnp.bfloat16)
    return lax.map(one_sequence, tokens)
```

```python
import functools

import jax
import jax.numpy as jnp
from jax import lax
from jax.experimental import pallas as pl
from jax.experimental.pallas import tpu as pltpu
from jax.sharding import PartitionSpec as P

GROUP = 4
LANES = 128
EDGE = 16


def kernel(depth_z, taps_count, tok_hbm, w_hbm, wo_hbm, taps_ref, gain_ref, bias_ref, out_ref,
           tok, wg, wo, gp, cs, call, act,
           load_sem, tok_s, tok_r, w_s, w_r, wd_s, wd_r, halo_s, halo_r,
           cv_s, cv_r, oz_s, oz_r, op_s, op_r, od_s, od_r):
    s, c = lax.axis_index("sp"), lax.axis_index("dp")
    q, z = s % GROUP, s // GROUP
    sx = s + 1 - 2 * (s % 2)
    sy = s + 2 - 4 * ((s // 2) % 2)
    sd = sx + 2 - 4 * ((sx // 2) % 2)
    qx, qy, qd = sx % GROUP, sy % GROUP, sd % GROUP
    rows, width = tok_hbm.shape
    krows = w_hbm.shape[0]
    orows, ocols = wo_hbm.shape
    steps = depth_z - 1
    span = GROUP * rows

    def remote(src, dst, ss, rs, sp, dp):
        return pltpu.make_async_remote_copy(
            src_ref=src, dst_ref=dst, send_sem=ss, recv_sem=rs,
            device_id={"sp": sp, "dp": dp}, device_id_type=pl.DeviceIdType.MESH)

    def tok_at(who, half):
        return tok.at[pl.ds(pl.multiple_of(who * rows + half * (rows // 2), rows // 2), rows // 2), :]

    def wg_at(core, zz):
        return wg.at[pl.ds(pl.multiple_of(core * krows, krows), krows),
                     pl.ds(pl.multiple_of(zz * LANES, LANES), LANES)]

    def wo_at(core, zz, who):
        return wo.at[pl.ds(pl.multiple_of(core * orows, orows), orows),
                     pl.ds(pl.multiple_of((zz * GROUP + who) * ocols, ocols), ocols)]

    def wo_half(core, zz, who, half):
        return wo.at[pl.ds(pl.multiple_of(core * orows + half * (orows // 2), orows // 2), orows // 2),
                     pl.ds(pl.multiple_of((zz * GROUP + who) * ocols, ocols), ocols)]

    def wo_plane(core, zz):
        return wo.at[pl.ds(pl.multiple_of(core * orows, orows), orows),
                     pl.ds(pl.multiple_of(zz * GROUP * ocols, GROUP * ocols), GROUP * ocols)]

    loads = [
        pltpu.make_async_copy(tok_hbm, tok.at[pl.ds(pl.multiple_of(q * rows, rows), rows), :], load_sem.at[0]),
        pltpu.make_async_copy(w_hbm, wg_at(c, z), load_sem.at[1]),
        pltpu.make_async_copy(wo_hbm, wo_at(c, z, q), load_sem.at[2]),
    ]
    for load in loads:
        load.start()
    barrier = pltpu.get_barrier_semaphore()

    def greet(sp, dp):
        pl.semaphore_signal(barrier, inc=1, device_id={"sp": sp, "dp": dp},
                            device_id_type=pl.DeviceIdType.MESH)

    for peer in (sx, sy, sd):
        greet(peer, c)
    greet(s, 1 - c)
    pl.when(z > 0)(lambda: greet(s - GROUP, c))
    pl.when(z < steps)(lambda: greet(s + GROUP, c))
    ends = (z == 0).astype(jnp.int32) + (z == steps).astype(jnp.int32)
    pl.semaphore_wait(barrier, 6 - ends)

    slots = [(0, z, None)]
    for step in range(steps):
        slots.append((1 + step, z - 1 - step, z - 1 - step >= 0))
        slots.append((1 + steps + step, z + 1 + step, z + 1 + step <= steps))
    slots_by = {slot[0]: slot for slot in slots}

    def guarded(cond, fn):
        if cond is None:
            fn()
        else:
            pl.when(cond)(fn)

    def z_send(at, ss, rs, step):
        up, down = z - step, z + step

        def go_up():
            remote(at(c, up), at(c, up), ss.at[0, step], rs.at[0, step], s + GROUP, c).start()

        def go_down():
            remote(at(c, down), at(c, down), ss.at[1, step], rs.at[1, step], s - GROUP, c).start()

        pl.when((up >= 0) & (z < steps))(go_up)
        pl.when((down <= steps) & (z > 0))(go_down)

    def z_send_wait(at, ss, rs, step):
        up, down = z - step, z + step
        pl.when((up >= 0) & (z < steps))(
            lambda: remote(at(c, up), at(c, up), ss.at[0, step], rs.at[0, step], s + GROUP, c).wait_send())
        pl.when((down <= steps) & (z > 0))(
            lambda: remote(at(c, down), at(c, down), ss.at[1, step], rs.at[1, step], s - GROUP, c).wait_send())

    def z_recv(at, ss, rs, step):
        lo, hi = z - 1 - step, z + 1 + step
        pl.when(lo >= 0)(
            lambda: remote(at(c, lo), at(c, lo), ss.at[0, step], rs.at[0, step], s - GROUP, c).wait_recv())
        pl.when(hi <= steps)(
            lambda: remote(at(c, hi), at(c, hi), ss.at[1, step], rs.at[1, step], s + GROUP, c).wait_recv())

    def w_cross(slot):
        index, zz, cond = slot
        guarded(cond, lambda: remote(wg_at(c, zz), wg_at(c, zz), wd_s.at[index], wd_r.at[index], s, 1 - c).start())

    def square_send(at, ss, rs):
        for kind, half, peer in ((0, 0, sx), (2, 1, sy), (1, 1, sx), (3, 0, sy)):
            remote(at(q, half), at(q, half), ss.at[kind], rs.at[kind], peer, c).start()

    def square_pass(at, ss, rs):
        remote(at(qx, 0), at(qx, 0), ss.at[0], rs.at[0], sx, c).wait_recv()
        remote(at(qx, 0), at(qx, 0), ss.at[4], rs.at[4], sy, c).start()
        remote(at(qy, 1), at(qy, 1), ss.at[2], rs.at[2], sy, c).wait_recv()
        remote(at(qy, 1), at(qy, 1), ss.at[5], rs.at[5], sx, c).start()

    def square_finish(at, ss, rs):
        for kind, who, half, peer in ((1, qx, 1, sx), (3, qy, 0, sy), (4, qd, 0, sy), (5, qd, 1, sx)):
            remote(at(who, half), at(who, half), ss.at[kind], rs.at[kind], peer, c).wait_recv()

    def square_sent(at, ss, rs):
        for kind, who, half, peer in ((0, q, 0, sx), (2, q, 1, sy), (1, q, 1, sx), (3, q, 0, sy),
                                      (4, qx, 0, sy), (5, qy, 1, sx)):
            remote(at(who, half), at(who, half), ss.at[kind], rs.at[kind], peer, c).wait_send()

    def o_args(slot):
        index, zz, cond = slot
        return (functools.partial(wo_half, c, zz), op_s.at[index], op_r.at[index])

    def own_wo(core, zz):
        return wo_at(core, zz, q)

    def o_cross(slot):
        index, zz, cond = slot
        return remote(wo_plane(c, zz), wo_plane(c, zz), od_s.at[index], od_r.at[index], s, 1 - c)

    loads[0].wait()
    square_send(tok_at, tok_s, tok_r)
    loads[1].wait()
    z_send(wg_at, w_s, w_r, 0)
    w_cross(slots_by[0])
    loads[2].wait()
    for step in range(steps):
        z_recv(wg_at, w_s, w_r, step)
        if step + 1 < steps:
            z_send(wg_at, w_s, w_r, step + 1)
        w_cross(slots_by[1 + step])
        w_cross(slots_by[1 + steps + step])
        if step == 0:
            square_pass(tok_at, tok_s, tok_r)
            square_send(*o_args(slots_by[0]))
        if step == steps - 2 or steps == 1:
            z_send(own_wo, oz_s, oz_r, 0)
    square_finish(tok_at, tok_s, tok_r)
    for index, zz, cond in slots:
        guarded(cond, lambda index=index, zz=zz: remote(
            wg_at(1 - c, zz), wg_at(1 - c, zz), wd_s.at[index], wd_r.at[index], s, 1 - c).wait_recv())

    tiles = depth_z // 2
    lane = lax.broadcasted_iota(jnp.int32, (1, LANES), 1) < LANES // 2

    def project(m, carry):
        cols = pl.ds(pl.multiple_of(m * 2 * LANES, 2 * LANES), 2 * LANES)
        both = jnp.dot(tok[...], wg[:, cols], preferred_element_type=jnp.float32)
        first, second = both[:, :LANES], both[:, LANES:]
        value = jnp.where(lane, first, pltpu.roll(second, LANES // 2, 1))
        gate = jnp.where(lane, pltpu.roll(first, LANES // 2, 1), second)
        gp[m, EDGE:EDGE + span, :] = (value * jax.nn.sigmoid(gate)).astype(jnp.bfloat16)
        return carry

    lax.fori_loop(0, tiles, project, 0)

    low_edge, high_edge = gp.at[:, 0:EDGE, :], gp.at[:, EDGE + span:, :]
    halo_up = lambda: remote(gp.at[:, span:EDGE + span, :], low_edge, halo_s.at[0], halo_r.at[0], s + GROUP, c)
    halo_down = lambda: remote(gp.at[:, EDGE:2 * EDGE, :], high_edge, halo_s.at[1], halo_r.at[1], s - GROUP, c)
    pl.when(z < steps)(lambda: halo_up().start())
    pl.when(z > 0)(lambda: halo_down().start())

    @pl.when(z == 0)
    def _():
        gp[:, 0:EDGE, :] = jnp.zeros((tiles, EDGE, LANES), gp.dtype)

    @pl.when(z == steps)
    def _():
        gp[:, EDGE + span:, :] = jnp.zeros((tiles, EDGE, LANES), gp.dtype)

    def o_arrive(step):
        z_recv(own_wo, oz_s, oz_r, step)
        if step + 1 < steps:
            z_send(own_wo, oz_s, oz_r, step + 1)
        for index in (1 + step, 1 + steps + step):
            guarded(slots_by[index][2], lambda index=index: square_send(*o_args(slots_by[index])))

    square_pass(*o_args(slots_by[0]))
    o_arrive(0)
    pl.when(z > 0)(lambda: halo_up().wait_recv())
    pl.when(z < steps)(lambda: halo_down().wait_recv())

    odd = (q % 2) == 1
    chunk = 64

    def convolve(i, carry):
        m, r = i // (span // chunk), i % (span // chunk)
        base = pl.multiple_of(m * 2 * GROUP * (LANES // 2) + (q // 2) * LANES, LANES)
        near = taps_ref[:, pl.ds(base, LANES)]
        far = taps_ref[:, pl.ds(pl.multiple_of(base + GROUP * (LANES // 2), LANES), LANES)]
        taps = jnp.where(lane, jnp.where(odd, pltpu.roll(near, LANES // 2, 1), near),
                         jnp.where(odd, far, pltpu.roll(far, LANES // 2, 1)))
        x = gp[m, pl.ds(pl.multiple_of(r * chunk, chunk), chunk + 2 * EDGE), :].astype(jnp.float32)
        total = jnp.zeros((chunk, LANES), jnp.float32)
        shift = EDGE - taps_count // 2
        for b in range(8):
            moved = x[b:b + chunk + 24]
            for a in range(4):
                k = 8 * a + b - shift
                if 0 <= k < taps_count:
                    total = total + taps[k:k + 1] * moved[8 * a:8 * a + chunk]
        cs[r // (rows // chunk), pl.ds(pl.multiple_of((r % (rows // chunk)) * chunk, chunk), chunk),
           pl.ds(pl.multiple_of(m * LANES, LANES), LANES)] = total.astype(jnp.bfloat16)
        return carry

    lax.fori_loop(0, tiles * (span // chunk), convolve, 0)

    sent = [remote(cs.at[who], call.at[q], cv_s.at[n], cv_r.at[n], peer, c)
            for n, (who, peer) in enumerate(((qd, sd), (qx, sx), (qy, sy)))]
    for copy in sent:
        copy.start()
    call[q] = cs[q]
    for step in range(1, steps):
        o_arrive(step)
    for slot in slots[1:3]:
        guarded(slot[2], lambda slot=slot: square_pass(*o_args(slot)))
    square_finish(*o_args(slots[0]))
    o_cross(slots[0]).start()
    for n, (who, peer) in enumerate(((qd, sd), (qx, sx), (qy, sy))):
        remote(cs.at[who], call.at[who], cv_s.at[n], cv_r.at[n], peer, c).wait_recv()

    channels = gain_ref.shape[1]
    pieces = []
    for t in range(channels // LANES):
        zz, pair = t // 2, 2 * (t % 2)
        a = call[pair, :, (zz // 2) * LANES:(zz // 2 + 1) * LANES].astype(jnp.float32)
        b = call[pair + 1, :, (zz // 2) * LANES:(zz // 2 + 1) * LANES].astype(jnp.float32)
        if zz % 2 == 0:
            pieces.append(jnp.where(lane, a, pltpu.roll(b, LANES // 2, 1)))
        else:
            pieces.append(jnp.where(lane, pltpu.roll(a, LANES // 2, 1), b))
    conv = jnp.concatenate(pieces, axis=1)
    mean = jnp.sum(conv, axis=1, keepdims=True) * (1.0 / channels)
    centred = conv - mean
    variance = jnp.sum(centred * centred, axis=1, keepdims=True) * (1.0 / channels)
    normed = centred * lax.rsqrt(variance + 1e-05) * gain_ref[...] + bias_ref[...]
    act[...] = (normed * jax.nn.sigmoid(normed)).astype(jnp.bfloat16)

    def finish(slot):
        index, zz, cond = slot
        remote(wo_plane(1 - c, zz), wo_plane(1 - c, zz), od_s.at[index], od_r.at[index], s, 1 - c).wait_recv()
        cols = pl.ds(pl.multiple_of(zz * GROUP * ocols, GROUP * ocols), GROUP * ocols)
        out_ref[:, cols] = jnp.dot(act[...], wo[:, cols], preferred_element_type=jnp.float32).astype(jnp.bfloat16)

    def gather(slot):
        square_finish(*o_args(slot))
        o_cross(slot).start()

    for n, slot in enumerate(slots):
        for later in slots[2 * n + 3:2 * n + 5] if n < steps else ():
            guarded(later[2], lambda later=later: square_pass(*o_args(later)))
        if n > 0:
            guarded(slot[2], lambda slot=slot: gather(slot))
    for slot in slots:
        guarded(slot[2], lambda slot=slot: finish(slot))

    square_sent(tok_at, tok_s, tok_r)
    for step in range(steps):
        z_send_wait(wg_at, w_s, w_r, step)
        z_send_wait(own_wo, oz_s, oz_r, step)
    pl.when(z < steps)(lambda: halo_up().wait_send())
    pl.when(z > 0)(lambda: halo_down().wait_send())
    for copy in sent:
        copy.wait_send()
    for slot in slots:
        def drain(slot=slot):
            index, zz, cond = slot
            remote(wg_at(c, zz), wg_at(c, zz), wd_s.at[index], wd_r.at[index], s, 1 - c).wait_send()
            square_sent(*o_args(slot))
            o_cross(slot).wait_send()
        guarded(slot[2], drain)


def fused(depth_z, tokens, w_value, w_gate, w_out, conv_taps, norm_gain, norm_bias):
    rows, width = tokens.shape[1:]
    krows = w_value.shape[0]
    orows, ocols = w_out.shape
    channels, taps_count = conv_taps.shape
    pair = jnp.concatenate([w_value, w_gate], axis=1)
    taps = jnp.pad(conv_taps.astype(jnp.float32).T, ((0, 2 * EDGE - taps_count), (0, 0)))
    steps, tiles, span = depth_z - 1, depth_z // 2, GROUP * rows
    slots = 1 + 2 * steps
    dma = pltpu.SemaphoreType.DMA
    near = pl.BlockSpec(memory_space=pltpu.VMEM)
    far = pl.BlockSpec(memory_space=pl.ANY)
    bf16 = jnp.bfloat16
    mixed = pl.pallas_call(
        functools.partial(kernel, depth_z, taps_count),
        out_shape=jax.ShapeDtypeStruct((rows, w_out.shape[1] * GROUP * depth_z), bf16),
        in_specs=[far, far, far, near, near, near],
        out_specs=near,
        scratch_shapes=[
            pltpu.VMEM((span, width), bf16),
            pltpu.VMEM((2 * krows, depth_z * LANES), bf16),
            pltpu.VMEM((2 * orows, depth_z * GROUP * ocols), bf16),
            pltpu.VMEM((tiles, span + 2 * EDGE, LANES), bf16),
            pltpu.VMEM((GROUP, rows, tiles * LANES), bf16),
            pltpu.VMEM((GROUP, rows, tiles * LANES), bf16),
            pltpu.VMEM((rows, channels), bf16),
            dma((3,)), dma((6,)), dma((6,)), dma((2, steps)), dma((2, steps)),
            dma((slots,)), dma((slots,)), dma((2,)), dma((2,)),
            dma((3,)), dma((3,)), dma((2, steps)), dma((2, steps)),
            dma((slots, 6)), dma((slots, 6)), dma((slots,)), dma((slots,)),
        ],
        compiler_params=pltpu.CompilerParams(collective_id=0, has_side_effects=True),
    )(tokens[0], pair, w_out, taps, norm_gain[None], norm_bias[None])
    return mixed[None]


def padded_2(block, sides, width):
    for axis, dim in sides:
        count = lax.axis_size(axis)
        forward = [(i, i + 1) for i in range(count - 1)]
        backward = [(target, source) for source, target in forward]
        low = lax.ppermute(
            lax.slice_in_dim(block, block.shape[dim] - width, None, axis=dim), axis, forward
        )
        high = lax.ppermute(lax.slice_in_dim(block, 0, width, axis=dim), axis, backward)
        block = jnp.concatenate([low, block, high], axis=dim)
    return block


def depthwise(padded, taps, length):
    weights = taps.astype(jnp.float32)
    total = jnp.zeros((padded.shape[0], length), jnp.float32)
    for offset in range(taps.shape[1]):
        total = total + weights[:, offset : offset + 1] * padded[
            :, offset : offset + length
        ].astype(jnp.float32)
    return total.astype(jnp.bfloat16)


def normalize(conv_tok, norm_gain, norm_bias):
    values = lax.optimization_barrier(conv_tok).astype(jnp.float32)
    mean = jnp.mean(values, axis=0, keepdims=True)
    centred = values - mean
    variance = jnp.mean(centred * centred, axis=0, keepdims=True)
    normed = centred * lax.rsqrt(variance + 1e-05) * norm_gain[:, None] + norm_bias[:, None]
    return (normed * jax.nn.sigmoid(normed)).astype(jnp.bfloat16)


def on_device(tokens, w_value, w_gate, w_out, conv_taps, norm_gain, norm_bias):
    rows = tokens[0]
    contract_rows = (((0,), (1,)), ((), ()))
    contract_first = (((0,), (0,)), ((), ()))
    value_cols, gate_cols, out_cols = (
        lax.all_gather(w_value, "dp", axis=0, tiled=True),
        lax.all_gather(w_gate, "dp", axis=0, tiled=True),
        lax.all_gather(w_out, "dp", axis=0, tiled=True),
    )
    pieces = lax.all_gather((value_cols, gate_cols), "sp", axis=1, tiled=True)
    value = lax.dot_general(pieces[0], rows, contract_rows, preferred_element_type=jnp.float32)
    gate = lax.dot_general(pieces[1], rows, contract_rows, preferred_element_type=jnp.float32)
    gated_t = (value * jax.nn.sigmoid(gate)).astype(jnp.bfloat16)
    margin = conv_taps.shape[1] // 2
    padded = padded_2(gated_t, (("sp", 1),), margin)
    conv_tok = depthwise(padded, conv_taps, gated_t.shape[1])
    act_t = normalize(conv_tok, norm_gain, norm_bias)
    mixed = lax.dot_general(
        act_t,
        lax.all_gather(out_cols, "sp", axis=1, tiled=True),
        contract_first,
        preferred_element_type=jnp.float32,
    )
    return mixed.astype(jnp.bfloat16)[None]


def on_any(tokens, w_value, w_gate, w_out, conv_taps, norm_gain, norm_bias):
    count, cores = lax.axis_size("sp"), lax.axis_size("dp")
    depth_z = count // GROUP
    fits = (cores == 2 and count % (2 * GROUP) == 0 and tokens.shape[0] == 1
            and 2 * w_value.shape[1] == LANES and w_out.shape[1] % LANES == 0
            and tokens.shape[1] % LANES == 0 and conv_taps.shape[1] // 2 < EDGE)
    args = (tokens, w_value, w_gate, w_out, conv_taps, norm_gain, norm_bias)
    return fused(depth_z, *args) if fits else on_device(*args)


def solution(mesh):
    in_specs = (P("dp", "sp", None), P("dp", "sp"), P("dp", "sp"), P("dp", "sp"), P(), P(), P())
    out_specs = P("dp", "sp", None)
    return jax.shard_map(
        on_any, mesh=mesh, in_specs=in_specs, out_specs=out_specs, check_vma=False
    )
```

```python
import functools

import jax
import jax.numpy as jnp
from jax import lax
from jax.experimental import pallas as pl
from jax.experimental.pallas import tpu as pltpu
from jax.sharding import PartitionSpec as P

GROUP = 4
LANES = 128
EDGE = 16


def kernel(depth_z, taps_count, tok_hbm, wv_hbm, wg_hbm, wo_hbm, taps_ref, gain_ref, bias_ref, out_ref,
           tok, wg, wo, gp, cs, call, act, tb,
           load_sem, tok_s, tok_r, w_s, w_r, wd_s, wd_r, halo_s, halo_r,
           cv_s, cv_r, oz_s, oz_r, op_s, op_r, od_s, od_r):
    s, c = lax.axis_index("sp"), lax.axis_index("dp")
    q, z = s % GROUP, s // GROUP
    sx = s + 1 - 2 * (s % 2)
    sy = s + 2 - 4 * ((s // 2) % 2)
    sd = sx + 2 - 4 * ((sx // 2) % 2)
    qx, qy, qd = sx % GROUP, sy % GROUP, sd % GROUP
    rows, width = tok_hbm.shape
    wcols, krows = wv_hbm.shape
    orows, ocols = wo_hbm.shape
    steps = depth_z - 1
    span = GROUP * rows

    def remote(src, dst, ss, rs, sp, dp):
        return pltpu.make_async_remote_copy(
            src_ref=src, dst_ref=dst, send_sem=ss, recv_sem=rs,
            device_id={"sp": sp, "dp": dp}, device_id_type=pl.DeviceIdType.MESH)

    def tok_at(who, half):
        return tok.at[pl.ds(pl.multiple_of(who * rows + half * (rows // 2), rows // 2), rows // 2), :]

    def wg_at(core, zz):
        return wg.at[:, pl.ds(pl.multiple_of(zz * wcols, wcols), wcols),
                     pl.ds(pl.multiple_of(core * krows, krows), krows)]

    def wo_at(core, zz, who):
        return wo.at[pl.ds(pl.multiple_of(core * orows, orows), orows),
                     pl.ds(pl.multiple_of((zz * GROUP + who) * ocols, ocols), ocols)]

    def wo_half(core, zz, who, half):
        return wo.at[pl.ds(pl.multiple_of(core * orows + half * (orows // 2), orows // 2), orows // 2),
                     pl.ds(pl.multiple_of((zz * GROUP + who) * ocols, ocols), ocols)]

    def wo_plane(core, zz):
        return wo.at[pl.ds(pl.multiple_of(core * orows, orows), orows),
                     pl.ds(pl.multiple_of(zz * GROUP * ocols, GROUP * ocols), GROUP * ocols)]

    loads = [
        pltpu.make_async_copy(tok_hbm, tok.at[pl.ds(pl.multiple_of(q * rows, rows), rows), :], load_sem.at[0]),
        pltpu.make_async_copy(wv_hbm, wg_at(c, z).at[0], load_sem.at[1]),
        pltpu.make_async_copy(wg_hbm, wg_at(c, z).at[1], load_sem.at[3]),
        pltpu.make_async_copy(wo_hbm, wo_at(c, z, q), load_sem.at[2]),
    ]
    for load in loads:
        load.start()
    barrier = pltpu.get_barrier_semaphore()

    def greet(sp, dp):
        pl.semaphore_signal(barrier, inc=1, device_id={"sp": sp, "dp": dp},
                            device_id_type=pl.DeviceIdType.MESH)

    for peer in (sx, sy, sd):
        greet(peer, c)
    greet(s, 1 - c)
    pl.when(z > 0)(lambda: greet(s - GROUP, c))
    pl.when(z < steps)(lambda: greet(s + GROUP, c))
    ends = (z == 0).astype(jnp.int32) + (z == steps).astype(jnp.int32)
    pl.semaphore_wait(barrier, 6 - ends)

    slots = [(0, z, None)]
    for step in range(steps):
        slots.append((1 + step, z - 1 - step, z - 1 - step >= 0))
        slots.append((1 + steps + step, z + 1 + step, z + 1 + step <= steps))
    slots_by = {slot[0]: slot for slot in slots}

    def guarded(cond, fn):
        if cond is None:
            fn()
        else:
            pl.when(cond)(fn)

    def z_send(at, ss, rs, step):
        up, down = z - step, z + step

        def go_up():
            remote(at(c, up), at(c, up), ss.at[0, step], rs.at[0, step], s + GROUP, c).start()

        def go_down():
            remote(at(c, down), at(c, down), ss.at[1, step], rs.at[1, step], s - GROUP, c).start()

        pl.when((up >= 0) & (z < steps))(go_up)
        pl.when((down <= steps) & (z > 0))(go_down)

    def z_send_wait(at, ss, rs, step):
        up, down = z - step, z + step
        pl.when((up >= 0) & (z < steps))(
            lambda: remote(at(c, up), at(c, up), ss.at[0, step], rs.at[0, step], s + GROUP, c).wait_send())
        pl.when((down <= steps) & (z > 0))(
            lambda: remote(at(c, down), at(c, down), ss.at[1, step], rs.at[1, step], s - GROUP, c).wait_send())

    def z_recv(at, ss, rs, step):
        lo, hi = z - 1 - step, z + 1 + step
        pl.when(lo >= 0)(
            lambda: remote(at(c, lo), at(c, lo), ss.at[0, step], rs.at[0, step], s - GROUP, c).wait_recv())
        pl.when(hi <= steps)(
            lambda: remote(at(c, hi), at(c, hi), ss.at[1, step], rs.at[1, step], s + GROUP, c).wait_recv())

    def w_cross(slot):
        index, zz, cond = slot
        guarded(cond, lambda: remote(wg_at(c, zz), wg_at(c, zz), wd_s.at[index], wd_r.at[index], s, 1 - c).start())

    def square_send(at, ss, rs):
        for kind, half, peer in ((0, 0, sx), (2, 1, sy), (1, 1, sx), (3, 0, sy)):
            remote(at(q, half), at(q, half), ss.at[kind], rs.at[kind], peer, c).start()

    def square_pass(at, ss, rs):
        remote(at(qx, 0), at(qx, 0), ss.at[0], rs.at[0], sx, c).wait_recv()
        remote(at(qx, 0), at(qx, 0), ss.at[4], rs.at[4], sy, c).start()
        remote(at(qy, 1), at(qy, 1), ss.at[2], rs.at[2], sy, c).wait_recv()
        remote(at(qy, 1), at(qy, 1), ss.at[5], rs.at[5], sx, c).start()

    def square_finish(at, ss, rs):
        for kind, who, half, peer in ((1, qx, 1, sx), (3, qy, 0, sy), (4, qd, 0, sy), (5, qd, 1, sx)):
            remote(at(who, half), at(who, half), ss.at[kind], rs.at[kind], peer, c).wait_recv()

    def square_sent(at, ss, rs):
        for kind, who, half, peer in ((0, q, 0, sx), (2, q, 1, sy), (1, q, 1, sx), (3, q, 0, sy),
                                      (4, qx, 0, sy), (5, qy, 1, sx)):
            remote(at(who, half), at(who, half), ss.at[kind], rs.at[kind], peer, c).wait_send()

    def o_args(slot):
        index, zz, cond = slot
        return (functools.partial(wo_half, c, zz), op_s.at[index], op_r.at[index])

    def own_wo(core, zz):
        return wo_at(core, zz, q)

    def o_cross(slot):
        index, zz, cond = slot
        return remote(wo_plane(c, zz), wo_plane(c, zz), od_s.at[index], od_r.at[index], s, 1 - c)

    loads[0].wait()
    square_send(tok_at, tok_s, tok_r)
    loads[1].wait()
    loads[2].wait()
    z_send(wg_at, w_s, w_r, 0)
    w_cross(slots_by[0])
    loads[3].wait()
    tiles = depth_z // 2
    lane = lax.broadcasted_iota(jnp.int32, (1, LANES), 1) < LANES // 2
    odd = (q % 2) == 1
    for m in range(tiles):
        base = pl.multiple_of(m * GROUP * LANES + (q // 2) * LANES, LANES)
        near = taps_ref[:, pl.ds(base, LANES)].astype(jnp.float32)
        far = taps_ref[:, pl.ds(pl.multiple_of(base + GROUP // 2 * LANES, LANES), LANES)].astype(jnp.float32)
        taps = jnp.where(lane, jnp.where(odd, pltpu.roll(near, LANES // 2, 1), near),
                         jnp.where(odd, far, pltpu.roll(far, LANES // 2, 1)))
        for k in range(taps_count):
            tb[m, k] = jnp.broadcast_to(taps[k:k + 1], (8, LANES))
    for step in range(steps):
        z_recv(wg_at, w_s, w_r, step)
        if step + 1 < steps:
            z_send(wg_at, w_s, w_r, step + 1)
        w_cross(slots_by[1 + step])
        w_cross(slots_by[1 + steps + step])
        if step == 0:
            square_pass(tok_at, tok_s, tok_r)
            square_send(*o_args(slots_by[0]))
        if step == steps - 2 or steps == 1:
            z_send(own_wo, oz_s, oz_r, 0)
    def o_line(step):
        z_recv(own_wo, oz_s, oz_r, step)
        if step + 1 < steps:
            z_send(own_wo, oz_s, oz_r, step + 1)
        each(step, lambda slot: square_send(*o_args(slot)))

    def each(step, fn):
        for index in (1 + step, 1 + steps + step):
            slot = slots_by[index]
            guarded(slot[2], lambda slot=slot: fn(slot))

    def o_pass(slot):
        square_pass(*o_args(slot))

    o_line(0)
    square_finish(tok_at, tok_s, tok_r)
    for index, zz, cond in slots:
        guarded(cond, lambda index=index, zz=zz: remote(
            wg_at(1 - c, zz), wg_at(1 - c, zz), wd_s.at[index], wd_r.at[index], s, 1 - c).wait_recv())

    def project(m, carry):
        cols = pl.ds(pl.multiple_of(m * LANES, LANES), LANES)
        across = (((1,), (1,)), ((), ()))
        value = lax.dot_general(tok[...], wg[0, cols, :], across, preferred_element_type=jnp.float32)
        gate = lax.dot_general(tok[...], wg[1, cols, :], across, preferred_element_type=jnp.float32)
        gp[m, EDGE:EDGE + span, :] = (value * jax.nn.sigmoid(gate)).astype(jnp.bfloat16)
        return carry

    lax.fori_loop(0, tiles, project, 0)

    low_edge, high_edge = gp.at[:, 0:EDGE, :], gp.at[:, EDGE + span:, :]
    halo_up = lambda: remote(gp.at[:, span:EDGE + span, :], low_edge, halo_s.at[0], halo_r.at[0], s + GROUP, c)
    halo_down = lambda: remote(gp.at[:, EDGE:2 * EDGE, :], high_edge, halo_s.at[1], halo_r.at[1], s - GROUP, c)
    pl.when(z < steps)(lambda: halo_up().start())
    pl.when(z > 0)(lambda: halo_down().start())

    @pl.when(z == 0)
    def _():
        gp[:, 0:EDGE, :] = jnp.zeros((tiles, EDGE, LANES), gp.dtype)

    @pl.when(z == steps)
    def _():
        gp[:, EDGE + span:, :] = jnp.zeros((tiles, EDGE, LANES), gp.dtype)

    chunk = 64
    chunks = span // chunk

    def convolve(m, r):
        x = gp[m, pl.ds(pl.multiple_of(r * chunk, chunk), chunk + 2 * EDGE), :].astype(jnp.float32)
        total = jnp.zeros((chunk // 8, 8, LANES), jnp.float32)
        shift = EDGE - taps_count // 2
        for b in range(8):
            moved = x[b:b + chunk + 24].reshape(chunk // 8 + 3, 8, LANES)
            for a in range(4):
                k = 8 * a + b - shift
                if 0 <= k < taps_count:
                    total = total + tb[m, k][None] * moved[a:a + chunk // 8]
        cs[r // (rows // chunk), pl.ds(pl.multiple_of((r % (rows // chunk)) * chunk, chunk), chunk),
           pl.ds(pl.multiple_of(m * LANES, LANES), LANES)] = total.reshape(chunk, LANES).astype(jnp.bfloat16)

    def inner(i, carry):
        convolve(i // (chunks - 2), i % (chunks - 2) + 1)
        return carry

    def outer(i, carry):
        convolve(i // 2, (i % 2) * (chunks - 1))
        return carry

    o_pass(slots[0])
    lax.fori_loop(0, tiles * (chunks - 2), inner, 0)
    pl.when(z > 0)(lambda: halo_up().wait_recv())
    pl.when(z < steps)(lambda: halo_down().wait_recv())
    lax.fori_loop(0, tiles * 2, outer, 0)

    sent = [remote(cs.at[who], call.at[q], cv_s.at[n], cv_r.at[n], peer, c)
            for n, (who, peer) in enumerate(((qd, sd), (qx, sx), (qy, sy)))]
    for copy in sent:
        copy.start()
    call[q] = cs[q]
    each(0, o_pass)
    for step in range(1, steps):
        o_line(step)
    square_finish(*o_args(slots[0]))
    o_cross(slots[0]).start()
    for n, (who, peer) in enumerate(((qd, sd), (qx, sx), (qy, sy))):
        remote(cs.at[who], call.at[who], cv_s.at[n], cv_r.at[n], peer, c).wait_recv()

    channels = gain_ref.shape[1]
    pieces = []
    for t in range(channels // LANES):
        zz, pair = t // 2, 2 * (t % 2)
        a = call[pair, :, (zz // 2) * LANES:(zz // 2 + 1) * LANES].astype(jnp.float32)
        b = call[pair + 1, :, (zz // 2) * LANES:(zz // 2 + 1) * LANES].astype(jnp.float32)
        if zz % 2 == 0:
            pieces.append(jnp.where(lane, a, pltpu.roll(b, LANES // 2, 1)))
        else:
            pieces.append(jnp.where(lane, pltpu.roll(a, LANES // 2, 1), b))
    conv = jnp.concatenate(pieces, axis=1)
    mean = jnp.sum(conv, axis=1, keepdims=True) * (1.0 / channels)
    centred = conv - mean
    variance = jnp.sum(centred * centred, axis=1, keepdims=True) * (1.0 / channels)
    normed = centred * lax.rsqrt(variance + 1e-05) * gain_ref[...] + bias_ref[...]
    act[...] = (normed * jax.nn.sigmoid(normed)).astype(jnp.bfloat16)

    def finish(slot):
        index, zz, cond = slot
        remote(wo_plane(1 - c, zz), wo_plane(1 - c, zz), od_s.at[index], od_r.at[index], s, 1 - c).wait_recv()
        cols = pl.ds(pl.multiple_of(zz * GROUP * ocols, GROUP * ocols), GROUP * ocols)
        out_ref[:, cols] = jnp.dot(act[...], wo[:, cols], preferred_element_type=jnp.float32).astype(jnp.bfloat16)

    def gather(slot):
        square_finish(*o_args(slot))
        o_cross(slot).start()

    finish(slots[0])
    for step in range(steps):
        if step + 1 < steps:
            each(step + 1, o_pass)
        each(step, gather)
        if step > 0:
            each(step - 1, finish)
    each(steps - 1, finish)

    square_sent(tok_at, tok_s, tok_r)
    for step in range(steps):
        z_send_wait(wg_at, w_s, w_r, step)
        z_send_wait(own_wo, oz_s, oz_r, step)
    pl.when(z < steps)(lambda: halo_up().wait_send())
    pl.when(z > 0)(lambda: halo_down().wait_send())
    for copy in sent:
        copy.wait_send()
    for slot in slots:
        def drain(slot=slot):
            index, zz, cond = slot
            remote(wg_at(c, zz), wg_at(c, zz), wd_s.at[index], wd_r.at[index], s, 1 - c).wait_send()
            square_sent(*o_args(slot))
            o_cross(slot).wait_send()
        guarded(slot[2], drain)


def fused(depth_z, tokens, w_value, w_gate, w_out, conv_taps, norm_gain, norm_bias):
    rows, width = tokens.shape[1:]
    krows = w_value.shape[0]
    orows, ocols = w_out.shape
    channels, taps_count = conv_taps.shape
    steps, tiles, span = depth_z - 1, depth_z // 2, GROUP * rows
    slots = 1 + 2 * steps
    dma = pltpu.SemaphoreType.DMA
    near = pl.BlockSpec(memory_space=pltpu.VMEM)
    far = pl.BlockSpec(memory_space=pl.ANY)
    bf16 = jnp.bfloat16
    mixed = pl.pallas_call(
        functools.partial(kernel, depth_z, taps_count),
        out_shape=pltpu.VMEM((rows, w_out.shape[1] * GROUP * depth_z), bf16),
        in_specs=[far, far, far, far, near, near, near],
        out_specs=near,
        scratch_shapes=[
            pltpu.VMEM((span, width), bf16),
            pltpu.VMEM((2, depth_z * w_value.shape[1], 2 * krows), bf16),
            pltpu.VMEM((2 * orows, depth_z * GROUP * ocols), bf16),
            pltpu.VMEM((tiles, span + 2 * EDGE, LANES), bf16),
            pltpu.VMEM((GROUP, rows, tiles * LANES), bf16),
            pltpu.VMEM((GROUP, rows, tiles * LANES), bf16),
            pltpu.VMEM((rows, channels), bf16),
            pltpu.VMEM((tiles, taps_count, 8, LANES), jnp.float32),
            dma((4,)), dma((6,)), dma((6,)), dma((2, steps)), dma((2, steps)),
            dma((slots,)), dma((slots,)), dma((2,)), dma((2,)),
            dma((3,)), dma((3,)), dma((2, steps)), dma((2, steps)),
            dma((slots, 6)), dma((slots, 6)), dma((slots,)), dma((slots,)),
        ],
        compiler_params=pltpu.CompilerParams(collective_id=0, has_side_effects=True),
    )(tokens[0], w_value.T, w_gate.T, w_out, conv_taps.T, norm_gain[None], norm_bias[None])
    return mixed[None]


def padded_2(block, sides, width):
    for axis, dim in sides:
        count = lax.axis_size(axis)
        forward = [(i, i + 1) for i in range(count - 1)]
        backward = [(target, source) for source, target in forward]
        low = lax.ppermute(
            lax.slice_in_dim(block, block.shape[dim] - width, None, axis=dim), axis, forward
        )
        high = lax.ppermute(lax.slice_in_dim(block, 0, width, axis=dim), axis, backward)
        block = jnp.concatenate([low, block, high], axis=dim)
    return block


def depthwise(padded, taps, length):
    weights = taps.astype(jnp.float32)
    total = jnp.zeros((padded.shape[0], length), jnp.float32)
    for offset in range(taps.shape[1]):
        total = total + weights[:, offset : offset + 1] * padded[
            :, offset : offset + length
        ].astype(jnp.float32)
    return total.astype(jnp.bfloat16)


def normalize(conv_tok, norm_gain, norm_bias):
    values = lax.optimization_barrier(conv_tok).astype(jnp.float32)
    mean = jnp.mean(values, axis=0, keepdims=True)
    centred = values - mean
    variance = jnp.mean(centred * centred, axis=0, keepdims=True)
    normed = centred * lax.rsqrt(variance + 1e-05) * norm_gain[:, None] + norm_bias[:, None]
    return (normed * jax.nn.sigmoid(normed)).astype(jnp.bfloat16)


def on_device(tokens, w_value, w_gate, w_out, conv_taps, norm_gain, norm_bias):
    rows = tokens[0]
    contract_rows = (((0,), (1,)), ((), ()))
    contract_first = (((0,), (0,)), ((), ()))
    value_cols, gate_cols, out_cols = (
        lax.all_gather(w_value, "dp", axis=0, tiled=True),
        lax.all_gather(w_gate, "dp", axis=0, tiled=True),
        lax.all_gather(w_out, "dp", axis=0, tiled=True),
    )
    pieces = lax.all_gather((value_cols, gate_cols), "sp", axis=1, tiled=True)
    value = lax.dot_general(pieces[0], rows, contract_rows, preferred_element_type=jnp.float32)
    gate = lax.dot_general(pieces[1], rows, contract_rows, preferred_element_type=jnp.float32)
    gated_t = (value * jax.nn.sigmoid(gate)).astype(jnp.bfloat16)
    margin = conv_taps.shape[1] // 2
    padded = padded_2(gated_t, (("sp", 1),), margin)
    conv_tok = depthwise(padded, conv_taps, gated_t.shape[1])
    act_t = normalize(conv_tok, norm_gain, norm_bias)
    mixed = lax.dot_general(
        act_t,
        lax.all_gather(out_cols, "sp", axis=1, tiled=True),
        contract_first,
        preferred_element_type=jnp.float32,
    )
    return mixed.astype(jnp.bfloat16)[None]


def on_any(tokens, w_value, w_gate, w_out, conv_taps, norm_gain, norm_bias):
    count, cores = lax.axis_size("sp"), lax.axis_size("dp")
    depth_z = count // GROUP
    fits = (cores == 2 and count % (2 * GROUP) == 0 and tokens.shape[0] == 1
            and 2 * w_value.shape[1] == LANES and w_out.shape[1] % LANES == 0
            and tokens.shape[1] % LANES == 0 and conv_taps.shape[1] // 2 < EDGE)
    args = (tokens, w_value, w_gate, w_out, conv_taps, norm_gain, norm_bias)
    return fused(depth_z, *args) if fits else on_device(*args)


def solution(mesh):
    in_specs = (P("dp", "sp", None), P("dp", "sp"), P("dp", "sp"), P("dp", "sp"), P(), P(), P())
    out_specs = P("dp", "sp", None)
    return jax.shard_map(
        on_any, mesh=mesh, in_specs=in_specs, out_specs=out_specs, check_vma=False
    )
```

```python
import functools

import jax
import jax.numpy as jnp
from jax import lax
from jax.experimental import pallas as pl
from jax.experimental.pallas import tpu as pltpu
from jax.sharding import PartitionSpec as P

GROUP = 4
LANES = 128
EDGE = 16


def kernel(depth_z, taps_count, tok_hbm, wv_hbm, wg_hbm, wo_hbm, taps_hbm, gain_hbm, bias_hbm, out_ref,
           tok, wg, wo, gp, cs, call, act, tb, taps_ref, gain_ref, bias_ref,
           load_sem, tok_s, tok_r, w_s, w_r, wd_s, wd_r, halo_s, halo_r,
           cv_s, cv_r, oz_s, oz_r, dz_s, dz_r, op_s, op_r, od_s, od_r):
    s, c = lax.axis_index("sp"), lax.axis_index("dp")
    q, z = s % GROUP, s // GROUP
    sx = s + 1 - 2 * (s % 2)
    sy = s + 2 - 4 * ((s // 2) % 2)
    sd = sx + 2 - 4 * ((sx // 2) % 2)
    qx, qy, qd = sx % GROUP, sy % GROUP, sd % GROUP
    rows, width = tok_hbm.shape
    wcols, krows = wv_hbm.shape
    orows, ocols = wo_hbm.shape
    steps = depth_z - 1
    span = GROUP * rows

    def remote(src, dst, ss, rs, sp, dp):
        return pltpu.make_async_remote_copy(
            src_ref=src, dst_ref=dst, send_sem=ss, recv_sem=rs,
            device_id={"sp": sp, "dp": dp}, device_id_type=pl.DeviceIdType.MESH)

    def tok_at(who, half):
        return tok.at[pl.ds(pl.multiple_of(who * rows + half * (rows // 2), rows // 2), rows // 2), :]

    def wg_at(core, zz):
        return wg.at[:, pl.ds(pl.multiple_of(zz * wcols, wcols), wcols),
                     pl.ds(pl.multiple_of(core * krows, krows), krows)]

    def wo_at(core, zz, who):
        return wo.at[pl.ds(pl.multiple_of(core * orows, orows), orows),
                     pl.ds(pl.multiple_of((zz * GROUP + who) * ocols, ocols), ocols)]

    def wo_half(core, zz, who, half):
        return wo.at[pl.ds(pl.multiple_of(core * orows + half * (orows // 2), orows // 2), orows // 2),
                     pl.ds(pl.multiple_of((zz * GROUP + who) * ocols, ocols), ocols)]

    def wo_plane(core, zz):
        return wo.at[pl.ds(pl.multiple_of(core * orows, orows), orows),
                     pl.ds(pl.multiple_of(zz * GROUP * ocols, GROUP * ocols), GROUP * ocols)]

    loads = [
        pltpu.make_async_copy(tok_hbm, tok.at[pl.ds(pl.multiple_of(q * rows, rows), rows), :], load_sem.at[0]),
        pltpu.make_async_copy(wv_hbm, wg_at(c, z).at[0], load_sem.at[1]),
        pltpu.make_async_copy(wg_hbm, wg_at(c, z).at[1], load_sem.at[3]),
        pltpu.make_async_copy(taps_hbm, taps_ref, load_sem.at[4]),
        pltpu.make_async_copy(gain_hbm, gain_ref, load_sem.at[5]),
        pltpu.make_async_copy(bias_hbm, bias_ref, load_sem.at[6]),
        pltpu.make_async_copy(wo_hbm, wo_at(c, z, q), load_sem.at[2]),
    ]
    for load in loads:
        load.start()
    barrier = pltpu.get_barrier_semaphore()

    def greet(sp, dp):
        pl.semaphore_signal(barrier, inc=1, device_id={"sp": sp, "dp": dp},
                            device_id_type=pl.DeviceIdType.MESH)

    for peer in (sx, sy, sd):
        greet(peer, c)
    greet(s, 1 - c)
    pl.when(z > 0)(lambda: greet(s - GROUP, c))
    pl.when(z < steps)(lambda: greet(s + GROUP, c))
    ends = (z == 0).astype(jnp.int32) + (z == steps).astype(jnp.int32)
    pl.semaphore_wait(barrier, 6 - ends)

    slots = [(0, z, None)]
    for step in range(steps):
        slots.append((1 + step, z - 1 - step, z - 1 - step >= 0))
        slots.append((1 + steps + step, z + 1 + step, z + 1 + step <= steps))
    slots_by = {slot[0]: slot for slot in slots}

    def guarded(cond, fn):
        if cond is None:
            fn()
        else:
            pl.when(cond)(fn)

    def z_send(at, ss, rs, step):
        up, down = z - step, z + step

        def go_up():
            remote(at(c, up), at(c, up), ss.at[0, step], rs.at[0, step], s + GROUP, c).start()

        def go_down():
            remote(at(c, down), at(c, down), ss.at[1, step], rs.at[1, step], s - GROUP, c).start()

        pl.when((up >= 0) & (z < steps))(go_up)
        pl.when((down <= steps) & (z > 0))(go_down)

    def z_send_wait(at, ss, rs, step):
        up, down = z - step, z + step
        pl.when((up >= 0) & (z < steps))(
            lambda: remote(at(c, up), at(c, up), ss.at[0, step], rs.at[0, step], s + GROUP, c).wait_send())
        pl.when((down <= steps) & (z > 0))(
            lambda: remote(at(c, down), at(c, down), ss.at[1, step], rs.at[1, step], s - GROUP, c).wait_send())

    def z_recv(at, ss, rs, step):
        lo, hi = z - 1 - step, z + 1 + step
        pl.when(lo >= 0)(
            lambda: remote(at(c, lo), at(c, lo), ss.at[0, step], rs.at[0, step], s - GROUP, c).wait_recv())
        pl.when(hi <= steps)(
            lambda: remote(at(c, hi), at(c, hi), ss.at[1, step], rs.at[1, step], s + GROUP, c).wait_recv())

    def w_cross(slot):
        index, zz, cond = slot
        guarded(cond, lambda: remote(wg_at(c, zz), wg_at(c, zz), wd_s.at[index], wd_r.at[index], s, 1 - c).start())

    def square_send(at, ss, rs):
        for kind, half, peer in ((0, 0, sx), (2, 1, sy), (1, 1, sx), (3, 0, sy)):
            remote(at(q, half), at(q, half), ss.at[kind], rs.at[kind], peer, c).start()

    def square_pass(at, ss, rs):
        remote(at(qx, 0), at(qx, 0), ss.at[0], rs.at[0], sx, c).wait_recv()
        remote(at(qx, 0), at(qx, 0), ss.at[4], rs.at[4], sy, c).start()
        remote(at(qy, 1), at(qy, 1), ss.at[2], rs.at[2], sy, c).wait_recv()
        remote(at(qy, 1), at(qy, 1), ss.at[5], rs.at[5], sx, c).start()

    def square_finish(at, ss, rs):
        for kind, who, half, peer in ((1, qx, 1, sx), (3, qy, 0, sy), (4, qd, 0, sy), (5, qd, 1, sx)):
            remote(at(who, half), at(who, half), ss.at[kind], rs.at[kind], peer, c).wait_recv()

    def square_sent(at, ss, rs):
        for kind, who, half, peer in ((0, q, 0, sx), (2, q, 1, sy), (1, q, 1, sx), (3, q, 0, sy),
                                      (4, qx, 0, sy), (5, qy, 1, sx)):
            remote(at(who, half), at(who, half), ss.at[kind], rs.at[kind], peer, c).wait_send()

    def o_args(slot):
        index, zz, cond = slot
        return (functools.partial(wo_half, c, zz), op_s.at[index], op_r.at[index])

    def own_wo(core, zz):
        return wo_at(core, zz, q)

    def far_wo(core, zz):
        return wo_at(core, zz, qd)

    def far_line(step):
        z_recv(far_wo, dz_s, dz_r, step)
        if step + 1 < steps:
            z_send(far_wo, dz_s, dz_r, step + 1)

    def sides_finish(at, ss, rs):
        for kind, who, half, peer in ((0, qx, 0, sx), (2, qy, 1, sy), (1, qx, 1, sx), (3, qy, 0, sy)):
            remote(at(who, half), at(who, half), ss.at[kind], rs.at[kind], peer, c).wait_recv()

    def sides_sent(at, ss, rs):
        for kind, half, peer in ((0, 0, sx), (2, 1, sy), (1, 1, sx), (3, 0, sy)):
            remote(at(q, half), at(q, half), ss.at[kind], rs.at[kind], peer, c).wait_send()

    def o_cross(slot):
        index, zz, cond = slot
        return remote(wo_plane(c, zz), wo_plane(c, zz), od_s.at[index], od_r.at[index], s, 1 - c)

    loads[0].wait()
    square_send(tok_at, tok_s, tok_r)
    loads[1].wait()
    loads[2].wait()
    z_send(wg_at, w_s, w_r, 0)
    w_cross(slots_by[0])
    for load in loads[3:]:
        load.wait()
    tiles = depth_z // 2
    lane = lax.broadcasted_iota(jnp.int32, (1, LANES), 1) < LANES // 2
    odd = (q % 2) == 1
    for m in range(tiles):
        base = pl.multiple_of(m * GROUP * LANES + (q // 2) * LANES, LANES)
        near = taps_ref[:, pl.ds(base, LANES)].astype(jnp.float32)
        far = taps_ref[:, pl.ds(pl.multiple_of(base + GROUP // 2 * LANES, LANES), LANES)].astype(jnp.float32)
        taps = jnp.where(lane, jnp.where(odd, pltpu.roll(near, LANES // 2, 1), near),
                         jnp.where(odd, far, pltpu.roll(far, LANES // 2, 1)))
        for k in range(taps_count):
            tb[m, k] = jnp.broadcast_to(taps[k:k + 1], (8, LANES))
    for step in range(steps):
        z_recv(wg_at, w_s, w_r, step)
        if step + 1 < steps:
            z_send(wg_at, w_s, w_r, step + 1)
        w_cross(slots_by[1 + step])
        w_cross(slots_by[1 + steps + step])
        if step == 0:
            square_pass(tok_at, tok_s, tok_r)
            square_send(*o_args(slots_by[0]))
        if step == steps - 2 or steps == 1:
            z_send(own_wo, oz_s, oz_r, 0)
    def o_line(step):
        z_recv(own_wo, oz_s, oz_r, step)
        if step + 1 < steps:
            z_send(own_wo, oz_s, oz_r, step + 1)
        each(step, lambda slot: square_send(*o_args(slot)))

    def each(step, fn):
        for index in (1 + step, 1 + steps + step):
            slot = slots_by[index]
            guarded(slot[2], lambda slot=slot: fn(slot))

    def o_pass(slot):
        square_pass(*o_args(slot))

    o_line(0)
    square_finish(tok_at, tok_s, tok_r)
    for index, zz, cond in slots:
        guarded(cond, lambda index=index, zz=zz: remote(
            wg_at(1 - c, zz), wg_at(1 - c, zz), wd_s.at[index], wd_r.at[index], s, 1 - c).wait_recv())

    def project(m, carry):
        cols = pl.ds(pl.multiple_of(m * LANES, LANES), LANES)
        across = (((1,), (1,)), ((), ()))
        value = lax.dot_general(tok[...], wg[0, cols, :], across, preferred_element_type=jnp.float32)
        gate = lax.dot_general(tok[...], wg[1, cols, :], across, preferred_element_type=jnp.float32)
        gp[m, EDGE:EDGE + span, :] = (value * jax.nn.sigmoid(gate)).astype(jnp.bfloat16)
        return carry

    lax.fori_loop(0, tiles, project, 0)

    low_edge, high_edge = gp.at[:, 0:EDGE, :], gp.at[:, EDGE + span:, :]
    halo_up = lambda: remote(gp.at[:, span:EDGE + span, :], low_edge, halo_s.at[0], halo_r.at[0], s + GROUP, c)
    halo_down = lambda: remote(gp.at[:, EDGE:2 * EDGE, :], high_edge, halo_s.at[1], halo_r.at[1], s - GROUP, c)
    pl.when(z < steps)(lambda: halo_up().start())
    pl.when(z > 0)(lambda: halo_down().start())

    @pl.when(z == 0)
    def _():
        gp[:, 0:EDGE, :] = jnp.zeros((tiles, EDGE, LANES), gp.dtype)

    @pl.when(z == steps)
    def _():
        gp[:, EDGE + span:, :] = jnp.zeros((tiles, EDGE, LANES), gp.dtype)

    chunk = 64
    chunks = span // chunk

    def convolve(m, r):
        x = gp[m, pl.ds(pl.multiple_of(r * chunk, chunk), chunk + 2 * EDGE), :].astype(jnp.float32)
        total = jnp.zeros((chunk // 8, 8, LANES), jnp.float32)
        shift = EDGE - taps_count // 2
        for b in range(8):
            moved = x[b:b + chunk + 24].reshape(chunk // 8 + 3, 8, LANES)
            for a in range(4):
                k = 8 * a + b - shift
                if 0 <= k < taps_count:
                    total = total + tb[m, k][None] * moved[a:a + chunk // 8]
        cs[r // (rows // chunk), pl.ds(pl.multiple_of((r % (rows // chunk)) * chunk, chunk), chunk),
           pl.ds(pl.multiple_of(m * LANES, LANES), LANES)] = total.reshape(chunk, LANES).astype(jnp.bfloat16)

    def inner(i, carry):
        convolve(i // (chunks - 2), i % (chunks - 2) + 1)
        return carry

    def outer(i, carry):
        convolve(i // 2, (i % 2) * (chunks - 1))
        return carry

    o_pass(slots[0])
    half = tiles * (chunks - 2) // 2
    lax.fori_loop(0, half, inner, 0)
    for step in range(1, min(2, steps)):
        o_line(step)
    square_finish(*o_args(slots[0]))
    z_send(far_wo, dz_s, dz_r, 0)
    o_cross(slots[0]).start()
    lax.fori_loop(half, tiles * (chunks - 2), inner, 0)
    pl.when(z > 0)(lambda: halo_up().wait_recv())
    pl.when(z < steps)(lambda: halo_down().wait_recv())
    lax.fori_loop(0, tiles * 2, outer, 0)

    sent = [remote(cs.at[who], call.at[q], cv_s.at[n], cv_r.at[n], peer, c)
            for n, (who, peer) in enumerate(((qd, sd), (qx, sx), (qy, sy)))]
    for copy in sent:
        copy.start()
    call[q] = cs[q]
    for step in range(2, steps):
        o_line(step)
    far_line(0)
    for n, (who, peer) in enumerate(((qd, sd), (qx, sx), (qy, sy))):
        remote(cs.at[who], call.at[who], cv_s.at[n], cv_r.at[n], peer, c).wait_recv()

    channels = gain_ref.shape[1]
    pieces = []
    for t in range(channels // LANES):
        zz, pair = t // 2, 2 * (t % 2)
        a = call[pair, :, (zz // 2) * LANES:(zz // 2 + 1) * LANES].astype(jnp.float32)
        b = call[pair + 1, :, (zz // 2) * LANES:(zz // 2 + 1) * LANES].astype(jnp.float32)
        if zz % 2 == 0:
            pieces.append(jnp.where(lane, a, pltpu.roll(b, LANES // 2, 1)))
        else:
            pieces.append(jnp.where(lane, pltpu.roll(a, LANES // 2, 1), b))
    conv = jnp.concatenate(pieces, axis=1)
    mean = jnp.sum(conv, axis=1, keepdims=True) * (1.0 / channels)
    centred = conv - mean
    variance = jnp.sum(centred * centred, axis=1, keepdims=True) * (1.0 / channels)
    normed = centred * lax.rsqrt(variance + 1e-05) * gain_ref[...] + bias_ref[...]
    act[...] = (normed * jax.nn.sigmoid(normed)).astype(jnp.bfloat16)

    def finish(slot):
        index, zz, cond = slot
        remote(wo_plane(1 - c, zz), wo_plane(1 - c, zz), od_s.at[index], od_r.at[index], s, 1 - c).wait_recv()
        cols = pl.ds(pl.multiple_of(zz * GROUP * ocols, GROUP * ocols), GROUP * ocols)
        out_ref[:, cols] = jnp.dot(act[...], wo[:, cols], preferred_element_type=jnp.float32).astype(jnp.bfloat16)

    def gather(slot):
        sides_finish(*o_args(slot))
        o_cross(slot).start()

    finish(slots[0])
    for step in range(steps):
        if step > 0:
            far_line(step)
        each(step, gather)
        if step > 0:
            each(step - 1, finish)
    each(steps - 1, finish)

    square_sent(tok_at, tok_s, tok_r)
    for step in range(steps):
        z_send_wait(wg_at, w_s, w_r, step)
        z_send_wait(own_wo, oz_s, oz_r, step)
        z_send_wait(far_wo, dz_s, dz_r, step)
    pl.when(z < steps)(lambda: halo_up().wait_send())
    pl.when(z > 0)(lambda: halo_down().wait_send())
    for copy in sent:
        copy.wait_send()
    for slot in slots:
        def drain(slot=slot):
            index, zz, cond = slot
            remote(wg_at(c, zz), wg_at(c, zz), wd_s.at[index], wd_r.at[index], s, 1 - c).wait_send()
            (square_sent if index == 0 else sides_sent)(*o_args(slot))
            o_cross(slot).wait_send()
        guarded(slot[2], drain)


def fused(depth_z, tokens, w_value, w_gate, w_out, conv_taps, norm_gain, norm_bias):
    rows, width = tokens.shape[1:]
    krows = w_value.shape[0]
    orows, ocols = w_out.shape
    channels, taps_count = conv_taps.shape
    steps, tiles, span = depth_z - 1, depth_z // 2, GROUP * rows
    slots = 1 + 2 * steps
    dma = pltpu.SemaphoreType.DMA
    near = pl.BlockSpec(memory_space=pltpu.VMEM)
    far = pl.BlockSpec(memory_space=pl.ANY)
    bf16 = jnp.bfloat16
    mixed = pl.pallas_call(
        functools.partial(kernel, depth_z, taps_count),
        out_shape=pltpu.VMEM((rows, w_out.shape[1] * GROUP * depth_z), bf16),
        in_specs=[far] * 7,
        out_specs=near,
        scratch_shapes=[
            pltpu.VMEM((span, width), bf16),
            pltpu.VMEM((2, depth_z * w_value.shape[1], 2 * krows), bf16),
            pltpu.VMEM((2 * orows, depth_z * GROUP * ocols), bf16),
            pltpu.VMEM((tiles, span + 2 * EDGE, LANES), bf16),
            pltpu.VMEM((GROUP, rows, tiles * LANES), bf16),
            pltpu.VMEM((GROUP, rows, tiles * LANES), bf16),
            pltpu.VMEM((rows, channels), bf16),
            pltpu.VMEM((tiles, taps_count, 8, LANES), jnp.float32),
            pltpu.VMEM(conv_taps.shape[::-1], bf16),
            pltpu.VMEM((1, channels), jnp.float32),
            pltpu.VMEM((1, channels), jnp.float32),
            dma((7,)), dma((6,)), dma((6,)), dma((2, steps)), dma((2, steps)),
            dma((slots,)), dma((slots,)), dma((2,)), dma((2,)),
            dma((3,)), dma((3,)), dma((2, steps)), dma((2, steps)), dma((2, steps)), dma((2, steps)),
            dma((slots, 6)), dma((slots, 6)), dma((slots,)), dma((slots,)),
        ],
        compiler_params=pltpu.CompilerParams(collective_id=0, has_side_effects=True),
    )(tokens[0], w_value.T, w_gate.T, w_out, conv_taps.T, norm_gain[None], norm_bias[None])
    return mixed[None]


def padded_2(block, sides, width):
    for axis, dim in sides:
        count = lax.axis_size(axis)
        forward = [(i, i + 1) for i in range(count - 1)]
        backward = [(target, source) for source, target in forward]
        low = lax.ppermute(
            lax.slice_in_dim(block, block.shape[dim] - width, None, axis=dim), axis, forward
        )
        high = lax.ppermute(lax.slice_in_dim(block, 0, width, axis=dim), axis, backward)
        block = jnp.concatenate([low, block, high], axis=dim)
    return block


def depthwise(padded, taps, length):
    weights = taps.astype(jnp.float32)
    total = jnp.zeros((padded.shape[0], length), jnp.float32)
    for offset in range(taps.shape[1]):
        total = total + weights[:, offset : offset + 1] * padded[
            :, offset : offset + length
        ].astype(jnp.float32)
    return total.astype(jnp.bfloat16)


def normalize(conv_tok, norm_gain, norm_bias):
    values = lax.optimization_barrier(conv_tok).astype(jnp.float32)
    mean = jnp.mean(values, axis=0, keepdims=True)
    centred = values - mean
    variance = jnp.mean(centred * centred, axis=0, keepdims=True)
    normed = centred * lax.rsqrt(variance + 1e-05) * norm_gain[:, None] + norm_bias[:, None]
    return (normed * jax.nn.sigmoid(normed)).astype(jnp.bfloat16)


def on_device(tokens, w_value, w_gate, w_out, conv_taps, norm_gain, norm_bias):
    rows = tokens[0]
    contract_rows = (((0,), (1,)), ((), ()))
    contract_first = (((0,), (0,)), ((), ()))
    value_cols, gate_cols, out_cols = (
        lax.all_gather(w_value, "dp", axis=0, tiled=True),
        lax.all_gather(w_gate, "dp", axis=0, tiled=True),
        lax.all_gather(w_out, "dp", axis=0, tiled=True),
    )
    pieces = lax.all_gather((value_cols, gate_cols), "sp", axis=1, tiled=True)
    value = lax.dot_general(pieces[0], rows, contract_rows, preferred_element_type=jnp.float32)
    gate = lax.dot_general(pieces[1], rows, contract_rows, preferred_element_type=jnp.float32)
    gated_t = (value * jax.nn.sigmoid(gate)).astype(jnp.bfloat16)
    margin = conv_taps.shape[1] // 2
    padded = padded_2(gated_t, (("sp", 1),), margin)
    conv_tok = depthwise(padded, conv_taps, gated_t.shape[1])
    act_t = normalize(conv_tok, norm_gain, norm_bias)
    mixed = lax.dot_general(
        act_t,
        lax.all_gather(out_cols, "sp", axis=1, tiled=True),
        contract_first,
        preferred_element_type=jnp.float32,
    )
    return mixed.astype(jnp.bfloat16)[None]


def on_any(tokens, w_value, w_gate, w_out, conv_taps, norm_gain, norm_bias):
    count, cores = lax.axis_size("sp"), lax.axis_size("dp")
    depth_z = count // GROUP
    fits = (cores == 2 and count % (2 * GROUP) == 0 and tokens.shape[0] == 1
            and 2 * w_value.shape[1] == LANES and w_out.shape[1] % LANES == 0
            and tokens.shape[1] % LANES == 0 and conv_taps.shape[1] // 2 < EDGE)
    args = (tokens, w_value, w_gate, w_out, conv_taps, norm_gain, norm_bias)
    return fused(depth_z, *args) if fits else on_device(*args)


def solution(mesh):
    in_specs = (P("dp", "sp", None), P("dp", "sp"), P("dp", "sp"), P("dp", "sp"), P(), P(), P())
    out_specs = P("dp", "sp", None)
    return jax.shard_map(
        on_any, mesh=mesh, in_specs=in_specs, out_specs=out_specs, check_vma=False
    )
```
